32 devices in a mesh: ep: 4 (over y, x), tp: 8 (over z, core).
Axes of the slice: x: 2, y: 2, z: 4, core: 2. Of those that a mesh axis runs over, the one named last changes fastest.
Arguments:
- query_heads: bfloat16 [1024, 2048], P('ep', 'tp'), may hold values from -60 to 60
- key_heads: bfloat16 [1024, 2048], P('ep', 'tp'), may hold values from -40.5 to 40.5
- value_heads: bfloat16 [1024, 2048], P('ep', 'tp'), may hold values from -6 to 6
- diff_lambda: float32 [16], P('tp'), may hold values from 0.3 to 0.8
- sub_gain: float32 [128], replicated, may hold values from 0.1 to 1.9
- out_weight: bfloat16 [2048, 4096], P('tp'), may hold values from -0.125 to 0.125
- routed_input: bfloat16 [1024, 4096], P('ep', 'tp'), may hold values from -40 to 40
- routes: int32 [1024, 2], P('ep'), may hold values from 0 to 3, all different within a row; in each aligned block of 256 rows (0 to 255, 256 to 511, ...) at most 256 rows name the same one
- route_weights: float32 [1024, 2], P('ep'), may hold values from 0.3 to 1.5
- expert_gate: bfloat16 [4, 4096, 4096], P('ep', None, 'tp'), may hold values from -0.09375 to 0.09375
- expert_up: bfloat16 [4, 4096, 4096], P('ep', None, 'tp'), may hold values from -0.09375 to 0.09375
- expert_down: bfloat16 [4, 4096, 4096], P('ep', 'tp'), may hold values from -0.09375 to 0.09375
- shared_gate: bfloat16 [4096, 2048], P(None, 'tp'), may hold values from -0.09375 to 0.09375
- shared_up: bfloat16 [4096, 2048], P(None, 'tp'), may hold values from -0.09375 to 0.09375
- shared_down: bfloat16 [2048, 4096], P('tp'), may hold values from -0.125 to 0.125
Outputs:
- mixer_output: bfloat16 [1024, 4096], P('ep', 'tp')
- routed_output: bfloat16 [1024, 4096], P('ep', 'tp')
The draws below stay inside these ranges and needn't reach their ends.
Inputs may be any that keep to these rules, and one draw needn't show every extreme that they name: `routes`: each row names 2 different experts. In each aligned block of 256 rows no expert is named by more than 256 rows, a bound that some block reaches.
All inputs are finite; a program needn't handle non-finite values.
Results may differ from the reference program's by a relative error of at most 0.02.
Values may be sent and summed in bfloat16 or wider, within the bound.
A program may use at most 128 MiB of HBM per device.

```python
import math
import jax
import jax.numpy as jnp
import numpy as np
from jax import lax

D = 4096
HEADS = 16
QK = 64
VD = 128
FF = 4096
FS = 2048
TOPK = 2
EXPERTS = 4
ROWS_B = 256
TOKENS_A = 1024
TOKENS_B = 1024
CAP = 256
N_EP = 4
N_TP = 8


def draw_query_heads(key, part):
    base_key = jax.random.fold_in(jax.random.fold_in(key, 11), 0)
    values = 1.3 * jnp.clip(jax.random.normal(base_key, (TOKENS_A, HEADS * 2 * QK), jnp.float32), -6.0, 6.0)
    return values.astype(jnp.bfloat16)


def draw_key_heads(key, part):
    base_key = jax.random.fold_in(jax.random.fold_in(key, 23), 0)
    values = 1.3 * jnp.clip(jax.random.normal(base_key, (TOKENS_A, HEADS * 2 * QK), jnp.float32), -6.0, 6.0)
    return values.astype(jnp.bfloat16)


def draw_routed_input(key, part):
    base_key, row_key = jax.random.split(jax.random.fold_in(key, 37))
    column_pos = jnp.arange(D, dtype=jnp.float32)[None, :] / D
    column_scale = 0.6 * jnp.exp(column_pos * jnp.log(3.0))
    row_scale = jnp.exp(jax.random.uniform(row_key, (TOKENS_B, 1), jnp.float32, jnp.log(0.7), jnp.log(1.4)))
    entries = jnp.clip(jax.random.normal(base_key, (TOKENS_B, D), jnp.float32), -6.0, 6.0)
    return (entries * column_scale * row_scale).astype(jnp.bfloat16)


def level_of(stream_key, shape, cuts, low, top_value):
    loudness = 1.0
    for axis_at, shards_of in cuts:
        draws = jax.random.uniform(jax.random.fold_in(jax.random.fold_in(stream_key, 6), axis_at), (shards_of,), jnp.float32, low / len(cuts), top_value / len(cuts))
        loudness = loudness * jnp.repeat(jnp.exp(draws), shape[axis_at] // shards_of).reshape((-1,) + (1,) * (len(shape) - 1 - axis_at))
    return loudness


def deal_out(rng, own, number, rows, amount, top, bound, lean):
    sequence = jax.random.permutation(rng, amount)
    heavy_load, common = shares(amount, rows * top, bound, lean, True), shares(amount, rows * top, bound, lean, False)
    places = jnp.arange(amount)

    def named(tallies, rotation):
        used = int((tallies > 0).sum())
        fixed = max(1, used // 4)
        passed = fixed + (places - fixed + rotation * (used - fixed)) % max(1, amount - fixed)
        return jnp.zeros((amount,), jnp.int32).at[sequence[jnp.where(places < fixed, places, passed)]].set(jnp.asarray(tallies, jnp.int32))

    tallies = jnp.where(number % 4 == 0, named(heavy_load, number // 4), named(common, number - number // 4 - 1))
    mixed = jax.random.permutation(jax.random.fold_in(own, 3), amount)
    giver, receiver = mixed[0:amount // 2 * 2:2], mixed[1:amount // 2 * 2:2]
    slack = jnp.minimum(tallies[giver] - 1, bound - tallies[receiver]) // 2
    slack = jnp.where((giver == sequence[0]) | (receiver == sequence[0]) | (tallies[receiver] == 0), 0, jnp.maximum(slack, 0))
    passed = jax.random.randint(jax.random.fold_in(own, 4), (amount // 2,), 0, 1 << 20) % (slack + 1)
    tallies = tallies.at[giver].add(-passed).at[receiver].add(passed)
    items = jnp.searchsorted(jnp.cumsum(tallies), jnp.arange(rows * top), side="right").astype(jnp.int32)
    grid = items.reshape(top, rows).T
    grid = grid[jax.random.permutation(jax.random.fold_in(own, 1), rows)]
    rotation = jax.random.randint(jax.random.fold_in(own, 2), (rows, 1), 0, top)
    return jnp.take_along_axis(grid, (jnp.arange(top)[None, :] + rotation) % top, axis=1)


def shares(amount, total, limit, skew, full):
    weights = [(1 << 20) // math.isqrt(rank ** skew) + 1 for rank in range(1, amount + 1)]
    largest = limit if full else min(limit, max(-(-total // amount), total * weights[0] // sum(weights)))
    least = 1 if total - largest >= amount - 1 else 0
    given, spare = [largest] + [least] * (amount - 1), total - largest - least * (amount - 1)
    while spare > 0:
        candidates = [i for i in range(1, amount) if given[i] < largest] or [i for i in range(1, amount) if given[i] < limit]
        pool, budget = sum([weights[i] for i in candidates]), spare
        for i in candidates:
            more = min(limit - given[i], max(1, budget * weights[i] // pool), spare)
            given[i] = given[i] + more
            spare = spare - more
    return np.array(given)


def normal_values(key, extent, deviation, bound, pieces=(), kind=jnp.bfloat16):
    drawn = jax.random.normal(key, extent, jnp.float32) * deviation
    if len(pieces) > 0:
        drawn = level_of(key, extent, pieces, -0.22, 0.18) * drawn
    return jnp.clip(drawn, min=-bound, max=bound).astype(kind)


def setup_inputs(seed: int = 0) -> dict:
    arg_keys = jax.random.split(jax.random.key(seed), 16)
    query_heads = draw_query_heads(jax.random.fold_in(arg_keys[15], 71), 0)
    key_heads = draw_key_heads(jax.random.fold_in(arg_keys[15], 71), 0)
    value_heads = normal_values(arg_keys[2], (TOKENS_A, HEADS * VD), 1.0, 6.0, ((0, 4), (1, 8)))
    diff_lambda = jnp.clip(0.3 + 0.5 * jax.random.uniform(arg_keys[3], (HEADS,), jnp.float32) ** level_of(arg_keys[3], (HEADS,), ((0, 8),), -0.2, 0.2), 0.3, 0.8)
    sub_gain = jnp.clip(1.0 + 0.18 * jax.random.normal(arg_keys[4], (VD,), jnp.float32), 0.1, 1.9)
    out_weight = normal_values(arg_keys[5], (HEADS * VD, D), (HEADS * VD) ** -0.5, 0.125, ((0, 8),))
    routed_input = draw_routed_input(jax.random.fold_in(arg_keys[15], 71), 0)
    routes_keys = jax.random.split(jax.random.fold_in(arg_keys[7], 1), TOKENS_B // ROWS_B)
    routes_turns = jax.random.permutation(jax.random.fold_in(arg_keys[7], 3), TOKENS_B // ROWS_B)
    routes = jax.vmap(lambda own, number: deal_out(jax.random.fold_in(arg_keys[7], 2), own, number, ROWS_B, EXPERTS, TOPK, CAP, 2))(routes_keys, routes_turns).reshape((TOKENS_B, TOPK))
    route_weights = jnp.clip(jnp.exp(math.log(1.5) - 1.60943787 * jax.random.uniform(arg_keys[8], (TOKENS_B, TOPK), jnp.float32) ** level_of(arg_keys[8], (TOKENS_B, TOPK), ((0, 4),), -0.2, 0.2)), 0.3, 1.5)
    expert_gate = normal_values(arg_keys[9], (EXPERTS, D, FF), D ** -0.5, 0.09375, ((0, 4), (2, 8)))
    expert_up = normal_values(arg_keys[10], (EXPERTS, D, FF), D ** -0.5, 0.09375, ((0, 4), (2, 8)))
    expert_down = normal_values(arg_keys[11], (EXPERTS, FF, D), FF ** -0.5, 0.09375, ((0, 4), (1, 8)))
    shared_gate = normal_values(arg_keys[12], (D, FS), D ** -0.5, 0.09375, ((1, 8),))
    shared_up = normal_values(arg_keys[13], (D, FS), D ** -0.5, 0.09375, ((1, 8),))
    shared_down = normal_values(arg_keys[14], (FS, D), FS ** -0.5, 0.125, ((0, 8),))
    return {"query_heads": query_heads, "key_heads": key_heads, "value_heads": value_heads, "diff_lambda": diff_lambda, "sub_gain": sub_gain, "out_weight": out_weight, "routed_input": routed_input, "routes": routes, "route_weights": route_weights, "expert_gate": expert_gate, "expert_up": expert_up, "expert_down": expert_down, "shared_gate": shared_gate, "shared_up": shared_up, "shared_down": shared_down}


ROPE_BASE = 10000.0
NORM_EPS = 1e-06
MASKED = -1e+30

def rotate(values, positions):
    half_width = values.shape[-1] // 2
    inverse_freq = ROPE_BASE ** (-jnp.arange(half_width, dtype=jnp.float32) / half_width)
    angles = positions.astype(jnp.float32)[:, None] * inverse_freq[None, :]
    angles = angles.reshape((angles.shape[0],) + (1,) * (values.ndim - 2) + (half_width,))
    cosine = jnp.cos(angles)
    sine_part = jnp.sin(angles)
    lower = values[..., :half_width]
    upper = values[..., half_width:]
    return jnp.concatenate([lower * cosine - upper * sine_part, upper * cosine + lower * sine_part], axis=-1)

def split_sum(left, right, groups):
    group_width = left.shape[1] // groups

    def add_group(summed, group_index):
        left_part = lax.dynamic_slice_in_dim(left, group_index * group_width, group_width, 1)
        right_part = lax.dynamic_slice_in_dim(right, group_index * group_width, group_width, 0)
        rounded = jnp.dot(left_part, right_part, preferred_element_type=jnp.float32).astype(jnp.bfloat16)
        rounded = lax.optimization_barrier(rounded)
        return (summed + rounded.astype(jnp.float32), None)
    start_sum = jnp.zeros((left.shape[0], right.shape[1]), jnp.float32)
    summed, _ = lax.scan(add_group, start_sum, jnp.arange(groups, dtype=jnp.int32))
    return summed

def attend_head(query_head, key_head, value_head, lambda_head, sub_gain):
    seq_len = query_head.shape[0]
    query_block = 512 if seq_len % 512 == 0 else seq_len
    score_scale = query_head.shape[-1] ** (-0.5)
    key_positions = jnp.arange(seq_len, dtype=jnp.int32)

    def one_block(block_index):
        block_start = block_index * query_block
        query_rows = lax.dynamic_slice_in_dim(query_head, block_start, query_block, 0)
        query_positions = block_start + jnp.arange(query_block, dtype=jnp.int32)
        visible = key_positions[None, :] <= query_positions[:, None]
        attended = []
        for which_map in range(2):
            scores = jnp.dot(query_rows[:, which_map], key_head[:, which_map].T, preferred_element_type=jnp.float32) * score_scale
            scores = jnp.where(visible, scores, MASKED)
            maxima = lax.optimization_barrier(jnp.max(scores, axis=1, keepdims=True))
            exp_weights = jnp.where(visible, jnp.exp(scores - maxima), 0.0)
            totals = lax.optimization_barrier(jnp.sum(exp_weights, axis=1, keepdims=True))
            weighted = jnp.dot(exp_weights.astype(jnp.bfloat16), value_head, preferred_element_type=jnp.float32)
            attended.append(weighted / totals)
        mixed_heads = attended[0] - lambda_head * attended[1]
        normed = mixed_heads * lax.rsqrt(lax.optimization_barrier(jnp.mean(mixed_heads * mixed_heads, axis=1, keepdims=True)) + NORM_EPS) * sub_gain
        return normed.astype(jnp.bfloat16)
    blocks = lax.map(one_block, jnp.arange(seq_len // query_block, dtype=jnp.int32))
    return blocks.reshape(seq_len, value_head.shape[1])

def expert_apply(token_rows, gate_weight, up_weight, down_weight):
    squares = lax.optimization_barrier(jnp.sum(jnp.square(token_rows.astype(jnp.float32)), axis=1, keepdims=True))
    factor = lax.rsqrt(squares / token_rows.shape[1] + NORM_EPS)
    gate_value = jnp.dot(token_rows, gate_weight, preferred_element_type=jnp.float32) * factor
    up_value = jnp.dot(token_rows, up_weight, preferred_element_type=jnp.float32) * factor
    hidden = (jax.nn.silu(gate_value) * up_value).astype(jnp.bfloat16)
    return split_sum(hidden, down_weight, N_TP)

def slot_table(routes, block_rows, capacity, experts):
    token_count, top_count = routes.shape
    block_total = token_count // block_rows
    grouped = routes.reshape(block_total, block_rows * top_count)
    onehot = (grouped[:, :, None] == jnp.arange(experts, dtype=jnp.int32)[None, None, :]).astype(jnp.int32)
    earlier = jnp.cumsum(onehot, axis=1) - onehot
    rank_within = lax.optimization_barrier(jnp.sum(earlier * onehot, axis=2))
    block_ids = jnp.arange(block_total, dtype=jnp.int32)[:, None]
    slot_index = grouped * (block_total * capacity) + block_ids * capacity + rank_within
    return slot_index.reshape(token_count * top_count)

def reference(query_heads, key_heads, value_heads, diff_lambda, sub_gain, out_weight, routed_input, routes, route_weights, expert_gate, expert_up, expert_down, shared_gate, shared_up, shared_down):
    seq_len = query_heads.shape[0]
    positions = jnp.arange(seq_len, dtype=jnp.int32)
    query_rot = rotate(query_heads.astype(jnp.float32).reshape(seq_len, HEADS, 2, QK), positions).astype(jnp.bfloat16)
    key_rot = rotate(key_heads.astype(jnp.float32).reshape(seq_len, HEADS, 2, QK), positions).astype(jnp.bfloat16)
    value_split = value_heads.reshape(seq_len, HEADS, VD)
    per_head = lax.map(lambda head_item: attend_head(head_item[0], head_item[1], head_item[2], head_item[3], sub_gain), (jnp.transpose(query_rot, (1, 0, 2, 3)), jnp.transpose(key_rot, (1, 0, 2, 3)), jnp.transpose(value_split, (1, 0, 2)), diff_lambda))
    heads_out = jnp.transpose(per_head, (1, 0, 2)).reshape(seq_len, HEADS * VD)
    mixer_output = split_sum(heads_out, out_weight, N_TP).astype(jnp.bfloat16)
    token_count = routed_input.shape[0]
    copies = token_count * TOPK
    slot_of_copy = slot_table(routes, ROWS_B, CAP, EXPERTS)
    per_expert = N_EP * CAP
    copy_token = jnp.arange(copies, dtype=jnp.int32) // TOPK
    token_table = jnp.zeros((EXPERTS * per_expert,), jnp.int32).at[slot_of_copy].set(copy_token)
    filled = jnp.zeros((EXPERTS * per_expert,), jnp.bfloat16).at[slot_of_copy].set(jnp.ones((copies,), jnp.bfloat16))
    gathered_rows = routed_input[token_table] * filled[:, None]
    expert_rows = gathered_rows.reshape(EXPERTS, per_expert, D)
    results = lax.map(lambda expert_item: expert_apply(expert_item[0], expert_item[1], expert_item[2], expert_item[3]), (expert_rows, expert_gate, expert_up, expert_down))
    results = results.astype(jnp.bfloat16).reshape(EXPERTS * per_expert, D)
    copy_results = results[slot_of_copy].reshape(token_count, TOPK, D)
    routed = lax.optimization_barrier(jnp.sum(copy_results.astype(jnp.float32) * route_weights[:, :, None], axis=1))
    shared_result = expert_apply(routed_input, shared_gate, shared_up, shared_down)
    routed_output = (routed + shared_result).astype(jnp.bfloat16)
    return (mixer_output, routed_output)
```

```python
import jax
import jax.numpy as jnp
from jax import lax
from jax.sharding import PartitionSpec as P

ROPE_BASE = 10000.0
NORM_EPS = 1e-06
MASKED = -1e30


def rotate(values, positions):
    half_width = values.shape[-1] // 2
    inverse_freq = ROPE_BASE ** (-jnp.arange(half_width, dtype=jnp.float32) / half_width)
    angles = positions.astype(jnp.float32)[:, None] * inverse_freq[None, :]
    angles = angles.reshape((angles.shape[0],) + (1,) * (values.ndim - 2) + (half_width,))
    cosine = jnp.cos(angles)
    sine_part = jnp.sin(angles)
    lower = values[..., :half_width]
    upper = values[..., half_width:]
    return jnp.concatenate(
        [lower * cosine - upper * sine_part, upper * cosine + lower * sine_part], axis=-1
    )


def mixer_terms(query_heads, key_heads, value_heads, diff_lambda, sub_gain, out_weight):
    row_count = query_heads.shape[0]
    local_heads = diff_lambda.shape[0]
    value_width = value_heads.shape[1] // local_heads
    key_width = query_heads.shape[1] // (2 * local_heads)
    score_scale = key_width ** (-0.5)
    offset = lax.axis_index("ep") * row_count
    positions = offset + jnp.arange(row_count, dtype=jnp.int32)
    last_row = offset + row_count - 1
    query_rot = rotate(
        query_heads.astype(jnp.float32).reshape(row_count, local_heads, 2, key_width), positions
    ).astype(jnp.bfloat16)
    queries = jnp.transpose(query_rot, (1, 2, 0, 3))
    key_rot = (
        rotate(
            key_heads.astype(jnp.float32).reshape(row_count, local_heads, 2, key_width), positions
        )
        .astype(jnp.bfloat16)
        .reshape(row_count, local_heads * 2 * key_width)
    )
    start_state = (
        jnp.full((local_heads, 2, row_count), MASKED, jnp.float32),
        jnp.zeros((local_heads, 2, row_count), jnp.float32),
        jnp.zeros((local_heads, 2, row_count, value_width), jnp.float32),
    )
    carried = start_state
    key_piece = lax.all_gather(key_rot, "ep", axis=0, tiled=True)
    value_piece = lax.all_gather(value_heads, "ep", axis=0, tiled=True)
    piece_rows = key_piece.shape[0]
    key_block = 512
    block_count = piece_rows // key_block
    key_blocks = key_piece.reshape(block_count, key_block, local_heads, 2, key_width)
    value_blocks = value_piece.reshape(block_count, key_block, local_heads, value_width)

    def block_step(running, block_item):
        key_rows, value_rows, block_index = block_item
        block_start = block_index * key_block

        def attend_block(partial_state):
            maxima, totals, weighted = partial_state
            key_positions = block_start + jnp.arange(key_block, dtype=jnp.int32)
            visible = key_positions[None, :] <= positions[:, None]
            scores = (
                jnp.einsum("hmqd,khmd->hmqk", queries, key_rows, preferred_element_type=jnp.float32)
                * score_scale
            )
            scores = jnp.where(visible, scores, MASKED)
            new_maxima = jnp.maximum(maxima, jnp.max(scores, axis=3))
            exp_weights = jnp.where(visible, jnp.exp(scores - new_maxima[..., None]), 0.0)
            shrink = jnp.exp(maxima - new_maxima)
            new_totals = totals * shrink + jnp.sum(exp_weights, axis=3)
            update = jnp.einsum(
                "hmqk,khw->hmqw",
                exp_weights.astype(jnp.bfloat16),
                value_rows,
                preferred_element_type=jnp.float32,
            )
            return (new_maxima, new_totals, weighted * shrink[..., None] + update)

        return (
            lax.cond(
                block_start <= last_row, attend_block, lambda partial_state: partial_state, running
            ),
            None,
        )

    carried, _ = lax.scan(
        block_step, carried, (key_blocks, value_blocks, jnp.arange(block_count, dtype=jnp.int32))
    )
    maxima, totals, weighted = carried
    attended = weighted / totals[..., None]
    mixed_heads = attended[:, 0] - diff_lambda[:, None, None] * attended[:, 1]
    normed = (
        mixed_heads
        * lax.rsqrt(jnp.mean(mixed_heads * mixed_heads, axis=2, keepdims=True) + NORM_EPS)
        * sub_gain
    )
    heads_out = jnp.transpose(normed.astype(jnp.bfloat16), (1, 0, 2)).reshape(
        row_count, local_heads * value_width
    )
    return jnp.dot(heads_out, out_weight, preferred_element_type=jnp.float32)


def expert_terms(
    routed_input, routes, expert_gate, expert_up, expert_down, shared_gate, shared_up, shared_down
):
    row_count, part_width = routed_input.shape
    top_count = routes.shape[1]
    local_experts = expert_gate.shape[0]
    groups = lax.axis_size("ep")
    experts = local_experts * groups
    capacity = 2 * row_count * top_count // experts
    copies = row_count * top_count
    flat_routes = routes.reshape(copies)
    onehot = (flat_routes[:, None] == jnp.arange(experts, dtype=jnp.int32)[None, :]).astype(
        jnp.int32
    )
    rank_within = jnp.sum((jnp.cumsum(onehot, axis=0) - onehot) * onehot, axis=1)
    slot_index = flat_routes * capacity + rank_within
    placer = (
        slot_index[:, None] == jnp.arange(experts * capacity, dtype=jnp.int32)[None, :]
    ).astype(jnp.bfloat16)
    token_slots = jnp.sum(placer.reshape(row_count, top_count, experts * capacity), axis=1)
    outgoing = jnp.dot(token_slots.T, routed_input, preferred_element_type=jnp.float32).astype(
        jnp.bfloat16
    )
    arrived = lax.all_to_all(
        outgoing.reshape(groups, local_experts * capacity, part_width),
        "ep",
        split_axis=0,
        concat_axis=0,
        tiled=True,
    )
    slot_count = groups * capacity
    slot_rows = jnp.transpose(
        arrived.reshape(groups, local_experts, capacity, part_width), (1, 0, 2, 3)
    ).reshape(local_experts, slot_count, part_width)
    slot_piece = lax.all_gather(slot_rows, "tp", axis=2, tiled=True)
    own_piece = lax.all_gather(routed_input[None], "tp", axis=2, tiled=True)
    own_rows = own_piece[0]
    gate_sum = jnp.einsum(
        "emc,ecf->emf", slot_piece, expert_gate, preferred_element_type=jnp.float32
    )
    up_sum = jnp.einsum("emc,ecf->emf", slot_piece, expert_up, preferred_element_type=jnp.float32)
    square_sum = jnp.sum(jnp.square(slot_piece.astype(jnp.float32)), axis=2)
    shared_gate_sum = jnp.dot(own_rows, shared_gate, preferred_element_type=jnp.float32)
    shared_up_sum = jnp.dot(own_rows, shared_up, preferred_element_type=jnp.float32)
    shared_square = jnp.sum(jnp.square(own_rows.astype(jnp.float32)), axis=1)
    full_width = expert_gate.shape[1]
    factor = lax.rsqrt(square_sum / full_width + NORM_EPS)[..., None]
    hidden = (jax.nn.silu(gate_sum * factor) * (up_sum * factor)).astype(jnp.bfloat16)
    shared_factor = lax.rsqrt(shared_square / full_width + NORM_EPS)[:, None]
    shared_hidden = (
        jax.nn.silu(shared_gate_sum * shared_factor) * (shared_up_sum * shared_factor)
    ).astype(jnp.bfloat16)
    shared_terms = jnp.dot(shared_hidden, shared_down, preferred_element_type=jnp.float32)
    routed_terms = jnp.einsum(
        "emf,efd->emd", hidden, expert_down, preferred_element_type=jnp.float32
    )
    routed_sum = lax.psum_scatter(
        routed_terms.astype(jnp.bfloat16), "tp", scatter_dimension=2, tiled=True
    ).astype(jnp.float32)
    return (routed_sum, shared_terms, placer)


def expert_finish(routed_sum, shared_sum, placer, route_weights):
    local_experts, slot_count, part_width = routed_sum.shape
    groups = lax.axis_size("ep")
    capacity = slot_count // groups
    leaving = jnp.transpose(
        routed_sum.astype(jnp.bfloat16).reshape(local_experts, groups, capacity, part_width),
        (1, 0, 2, 3),
    ).reshape(groups, local_experts * capacity, part_width)
    returned = lax.all_to_all(leaving, "ep", split_axis=0, concat_axis=0, tiled=True)
    copy_results = jnp.dot(
        placer,
        returned.reshape(groups * local_experts * capacity, part_width),
        preferred_element_type=jnp.float32,
    )
    row_count, top_count = route_weights.shape
    routed = jnp.sum(
        copy_results.reshape(row_count, top_count, part_width) * route_weights[:, :, None], axis=1
    )
    return (routed + shared_sum).astype(jnp.bfloat16)


def body(
    query_heads,
    key_heads,
    value_heads,
    diff_lambda,
    sub_gain,
    out_weight,
    routed_input,
    routes,
    route_weights,
    expert_gate,
    expert_up,
    expert_down,
    shared_gate,
    shared_up,
    shared_down,
):
    mixer_partial = mixer_terms(
        query_heads, key_heads, value_heads, diff_lambda, sub_gain, out_weight
    )
    routed_sum, shared_terms, placer = expert_terms(
        routed_input,
        routes,
        expert_gate,
        expert_up,
        expert_down,
        shared_gate,
        shared_up,
        shared_down,
    )
    mixer_sum, shared_sum = (
        lax.psum_scatter(
            mixer_partial.astype(jnp.bfloat16), "tp", scatter_dimension=1, tiled=True
        ).astype(jnp.float32),
        lax.psum_scatter(
            shared_terms.astype(jnp.bfloat16), "tp", scatter_dimension=1, tiled=True
        ).astype(jnp.float32),
    )
    return (
        mixer_sum.astype(jnp.bfloat16),
        expert_finish(routed_sum, shared_sum, placer, route_weights),
    )


def exchange(value, axis, swap):
    count = lax.axis_size(axis)
    return lax.ppermute(value, axis, [(i, swap(i)) for i in range(count)])


def to_partner(value):
    return exchange(value, "tp", lambda i: i ^ 1)


def along_z(value, step):
    return exchange(value, "tp", lambda i: i ^ (2 * step))


def along_ep(value, step):
    return exchange(value, "ep", lambda i: i ^ step)


def f32(value):
    return value.astype(jnp.float32)


def low(value):
    return value.astype(jnp.bfloat16)


def pair_sum(part):
    half = part.shape[0] // 2
    return f32(part[:half]) + f32(to_partner(part[half:]))


def z_sum(own, core):
    chips = lax.axis_size("tp") // 2
    chip = lax.axis_index("tp") // 2
    rows, width = own.shape
    wide = width // chips
    own = low(own)
    pieces = [
        along_z(lax.dynamic_slice(own, (0, (chip ^ step) * wide), (rows, wide)), step)
        for step in range(1, chips)
    ]
    total = f32(lax.dynamic_slice(own, (0, chip * wide), (rows, wide)))
    for piece in pieces:
        total = total + f32(piece)
    total = low(total)
    narrow = wide // 2
    other = to_partner(lax.dynamic_slice(total, (0, (1 - core) * narrow), (rows, narrow)))
    mine = lax.dynamic_slice(total, (0, core * narrow), (rows, narrow))
    first = jnp.where(core == 0, mine, other)
    second = jnp.where(core == 0, other, mine)
    return jnp.concatenate([first, second], axis=0)


def turn(value, core):
    half = value.shape[0] // 2
    first, second = value[:half], value[half:]
    return jnp.concatenate(
        [jnp.where(core == 0, first, second), jnp.where(core == 0, second, first)], axis=0
    )


def attend(query_heads, key_heads, value_heads, diff_lambda, sub_gain):
    row_count = query_heads.shape[0]
    local_heads = diff_lambda.shape[0]
    value_width = value_heads.shape[1] // local_heads
    key_width = query_heads.shape[1] // (2 * local_heads)
    groups = lax.axis_size("ep")
    index = lax.axis_index("ep")
    steps = jnp.arange(row_count, dtype=jnp.int32)
    positions = index * row_count + steps
    both = jnp.concatenate([query_heads, key_heads], axis=1)
    turned = low(
        rotate(f32(both).reshape(row_count, 4 * local_heads, key_width), positions)
    ).reshape(row_count, 4 * local_heads * key_width)
    query_rot = turned[:, : 2 * local_heads * key_width]
    own = jnp.concatenate([turned[:, 2 * local_heads * key_width :], value_heads], axis=1)
    blocks = [own] + [along_ep(own, step) for step in range(1, groups)]
    keys = jnp.concatenate(blocks, axis=0)
    key_positions = jnp.concatenate(
        [(index ^ step) * row_count + steps for step in range(groups)], axis=0
    )
    visible = key_positions[None, :] <= positions[:, None]
    outs = []
    value_start = 2 * local_heads * key_width
    for head in range(local_heads):
        values = keys[:, value_start + head * value_width : value_start + (head + 1) * value_width]
        maps = []
        for side in range(2):
            at = (2 * head + side) * key_width
            scores = lax.dot_general(
                query_rot[:, at : at + key_width],
                keys[:, at : at + key_width],
                (((1,), (1,)), ((), ())),
                preferred_element_type=jnp.float32,
            ) * (key_width ** (-0.5))
            scores = jnp.where(visible, scores, MASKED)
            maxima = jnp.max(scores, axis=1, keepdims=True)
            weights = jnp.exp(scores - maxima)
            totals = jnp.sum(weights, axis=1, keepdims=True)
            maps.append(
                jnp.dot(low(weights), values, preferred_element_type=jnp.float32) / totals
            )
        mixed = maps[0] - diff_lambda[head] * maps[1]
        outs.append(
            low(
                mixed
                * lax.rsqrt(jnp.mean(mixed * mixed, axis=1, keepdims=True) + NORM_EPS)
                * sub_gain
            )
        )
    return jnp.concatenate(outs, axis=1)


def gated(rows, gate, up, factor):
    gate_sum = jnp.dot(rows, gate, preferred_element_type=jnp.float32)
    up_sum = jnp.dot(rows, up, preferred_element_type=jnp.float32)
    return low(jax.nn.silu(gate_sum * factor) * (up_sum * factor))


def row_factor(rows):
    return lax.rsqrt(jnp.mean(jnp.square(f32(rows)), axis=1, keepdims=True) + NORM_EPS)


def dense_body(
    query_heads,
    key_heads,
    value_heads,
    diff_lambda,
    sub_gain,
    out_weight,
    routed_input,
    routes,
    route_weights,
    expert_gate,
    expert_up,
    expert_down,
    shared_gate,
    shared_up,
    shared_down,
):
    row_count, part_width = routed_input.shape
    half = row_count // 2
    quarter = half // 2
    chips = lax.axis_size("tp") // 2
    tp_index = lax.axis_index("tp")
    core, chip = tp_index % 2, tp_index // 2
    index = lax.axis_index("ep")
    gate, up, down = expert_gate[0], expert_up[0], expert_down[0]

    held = [routed_input] + [along_z(routed_input, step) for step in range(1, chips)]
    pairs = []
    for piece in held:
        other = to_partner(piece)
        pairs.append((jnp.where(core == 0, piece, other), jnp.where(core == 0, other, piece)))
    columns = []
    for place in range(chips):
        for side in range(2):
            chosen = pairs[0][side]
            for step in range(1, chips):
                chosen = jnp.where((chip ^ step) == place, pairs[step][side], chosen)
            columns.append(chosen)
    own = turn(jnp.concatenate(columns, axis=1), core)

    def share(step):
        picked = jnp.sum(jnp.where(routes == (index ^ step), route_weights, 0.0), axis=1)
        picked = turn(picked, core)
        return (along_ep(picked, step) if step else picked)[:, None]

    shares = [share(step) for step in range(4)]

    own_half = own[:half]
    x_half = along_ep(own_half, 1)
    y_half = along_ep(own_half, 2)
    d_first = along_ep(x_half[:quarter], 2)
    d_second = along_ep(y_half[quarter:], 1)
    d_half = jnp.concatenate([d_first, d_second], axis=0)

    heads_out = attend(query_heads, key_heads, value_heads, diff_lambda, sub_gain)
    mixer_part = low(jnp.dot(turn(heads_out, core), out_weight, preferred_element_type=jnp.float32))
    mixer_output = z_sum(pair_sum(mixer_part), core)

    def routed(rows, weight):
        hidden = gated(rows, gate, up, row_factor(rows))
        return jnp.dot(hidden, down, preferred_element_type=jnp.float32) * weight

    def remote(part, weight):
        rows = jnp.concatenate([part, to_partner(part)], axis=0)
        return pair_sum(low(routed(rows, weight)))

    shared_hidden = gated(own, shared_gate, shared_up, row_factor(own))
    shared_part = jnp.dot(shared_hidden, shared_down, preferred_element_type=jnp.float32)
    own_sum = pair_sum(low(routed(own, shares[0]) + shared_part))
    x_sum = remote(x_half, shares[1])
    y_sum = remote(y_half, shares[2])
    x_first = along_ep(low(x_sum[:quarter]), 1)
    y_second = along_ep(low(y_sum[quarter:]), 2)
    d_sum = low(remote(d_half, shares[3]))
    y_more = along_ep(d_sum[:quarter], 1)
    x_more = along_ep(d_sum[quarter:], 2)
    y_first = along_ep(low(y_sum[:quarter] + f32(y_more)), 2)
    x_second = along_ep(low(x_sum[quarter:] + f32(x_more)), 1)
    from_x = jnp.concatenate([x_first, x_second], axis=0)
    from_y = jnp.concatenate([y_first, y_second], axis=0)
    routed_output = z_sum(own_sum + f32(from_x) + f32(from_y), core)
    return mixer_output, routed_output


def power_of_two(value):
    return value & (value - 1) == 0


def solution(mesh):
    dense = mesh.shape["ep"] == 4 and mesh.shape["tp"] % 2 == 0 and power_of_two(mesh.shape["tp"])

    def chosen(*arguments):
        fits = dense and arguments[9].shape[0] == 1 and arguments[6].shape[0] % 32 == 0
        return (dense_body if fits else body)(*arguments)

    placed = (
        P("ep", "tp"),
        P("ep", "tp"),
        P("ep", "tp"),
        P("tp"),
        P(),
        P("tp", None),
        P("ep", "tp"),
        P("ep", None),
        P("ep", None),
        P("ep", None, "tp"),
        P("ep", None, "tp"),
        P("ep", "tp", None),
        P(None, "tp"),
        P(None, "tp"),
        P("tp", None),
    )
    return jax.shard_map(
        chosen, mesh=mesh, in_specs=placed, out_specs=(P("ep", "tp"), P("ep", "tp")), check_vma=False
    )
```

```python
import jax
import jax.numpy as jnp
from jax import lax
from jax.sharding import PartitionSpec as P

ROPE_BASE = 10000.0
NORM_EPS = 1e-06
MASKED = -1e30


def rotate(values, positions):
    half_width = values.shape[-1] // 2
    inverse_freq = ROPE_BASE ** (-jnp.arange(half_width, dtype=jnp.float32) / half_width)
    angles = positions.astype(jnp.float32)[:, None] * inverse_freq[None, :]
    angles = angles.reshape((angles.shape[0],) + (1,) * (values.ndim - 2) + (half_width,))
    cosine = jnp.cos(angles)
    sine_part = jnp.sin(angles)
    lower = values[..., :half_width]
    upper = values[..., half_width:]
    return jnp.concatenate(
        [lower * cosine - upper * sine_part, upper * cosine + lower * sine_part], axis=-1
    )


def mixer_terms(query_heads, key_heads, value_heads, diff_lambda, sub_gain, out_weight):
    row_count = query_heads.shape[0]
    local_heads = diff_lambda.shape[0]
    value_width = value_heads.shape[1] // local_heads
    key_width = query_heads.shape[1] // (2 * local_heads)
    score_scale = key_width ** (-0.5)
    offset = lax.axis_index("ep") * row_count
    positions = offset + jnp.arange(row_count, dtype=jnp.int32)
    last_row = offset + row_count - 1
    query_rot = rotate(
        query_heads.astype(jnp.float32).reshape(row_count, local_heads, 2, key_width), positions
    ).astype(jnp.bfloat16)
    queries = jnp.transpose(query_rot, (1, 2, 0, 3))
    key_rot = (
        rotate(
            key_heads.astype(jnp.float32).reshape(row_count, local_heads, 2, key_width), positions
        )
        .astype(jnp.bfloat16)
        .reshape(row_count, local_heads * 2 * key_width)
    )
    start_state = (
        jnp.full((local_heads, 2, row_count), MASKED, jnp.float32),
        jnp.zeros((local_heads, 2, row_count), jnp.float32),
        jnp.zeros((local_heads, 2, row_count, value_width), jnp.float32),
    )
    carried = start_state
    key_piece = lax.all_gather(key_rot, "ep", axis=0, tiled=True)
    value_piece = lax.all_gather(value_heads, "ep", axis=0, tiled=True)
    piece_rows = key_piece.shape[0]
    key_block = 512
    block_count = piece_rows // key_block
    key_blocks = key_piece.reshape(block_count, key_block, local_heads, 2, key_width)
    value_blocks = value_piece.reshape(block_count, key_block, local_heads, value_width)

    def block_step(running, block_item):
        key_rows, value_rows, block_index = block_item
        block_start = block_index * key_block

        def attend_block(partial_state):
            maxima, totals, weighted = partial_state
            key_positions = block_start + jnp.arange(key_block, dtype=jnp.int32)
            visible = key_positions[None, :] <= positions[:, None]
            scores = (
                jnp.einsum("hmqd,khmd->hmqk", queries, key_rows, preferred_element_type=jnp.float32)
                * score_scale
            )
            scores = jnp.where(visible, scores, MASKED)
            new_maxima = jnp.maximum(maxima, jnp.max(scores, axis=3))
            exp_weights = jnp.where(visible, jnp.exp(scores - new_maxima[..., None]), 0.0)
            shrink = jnp.exp(maxima - new_maxima)
            new_totals = totals * shrink + jnp.sum(exp_weights, axis=3)
            update = jnp.einsum(
                "hmqk,khw->hmqw",
                exp_weights.astype(jnp.bfloat16),
                value_rows,
                preferred_element_type=jnp.float32,
            )
            return (new_maxima, new_totals, weighted * shrink[..., None] + update)

        return (
            lax.cond(
                block_start <= last_row, attend_block, lambda partial_state: partial_state, running
            ),
            None,
        )

    carried, _ = lax.scan(
        block_step, carried, (key_blocks, value_blocks, jnp.arange(block_count, dtype=jnp.int32))
    )
    maxima, totals, weighted = carried
    attended = weighted / totals[..., None]
    mixed_heads = attended[:, 0] - diff_lambda[:, None, None] * attended[:, 1]
    normed = (
        mixed_heads
        * lax.rsqrt(jnp.mean(mixed_heads * mixed_heads, axis=2, keepdims=True) + NORM_EPS)
        * sub_gain
    )
    heads_out = jnp.transpose(normed.astype(jnp.bfloat16), (1, 0, 2)).reshape(
        row_count, local_heads * value_width
    )
    return jnp.dot(heads_out, out_weight, preferred_element_type=jnp.float32)


def expert_terms(
    routed_input, routes, expert_gate, expert_up, expert_down, shared_gate, shared_up, shared_down
):
    row_count, part_width = routed_input.shape
    top_count = routes.shape[1]
    local_experts = expert_gate.shape[0]
    groups = lax.axis_size("ep")
    experts = local_experts * groups
    capacity = 2 * row_count * top_count // experts
    copies = row_count * top_count
    flat_routes = routes.reshape(copies)
    onehot = (flat_routes[:, None] == jnp.arange(experts, dtype=jnp.int32)[None, :]).astype(
        jnp.int32
    )
    rank_within = jnp.sum((jnp.cumsum(onehot, axis=0) - onehot) * onehot, axis=1)
    slot_index = flat_routes * capacity + rank_within
    placer = (
        slot_index[:, None] == jnp.arange(experts * capacity, dtype=jnp.int32)[None, :]
    ).astype(jnp.bfloat16)
    token_slots = jnp.sum(placer.reshape(row_count, top_count, experts * capacity), axis=1)
    outgoing = jnp.dot(token_slots.T, routed_input, preferred_element_type=jnp.float32).astype(
        jnp.bfloat16
    )
    arrived = lax.all_to_all(
        outgoing.reshape(groups, local_experts * capacity, part_width),
        "ep",
        split_axis=0,
        concat_axis=0,
        tiled=True,
    )
    slot_count = groups * capacity
    slot_rows = jnp.transpose(
        arrived.reshape(groups, local_experts, capacity, part_width), (1, 0, 2, 3)
    ).reshape(local_experts, slot_count, part_width)
    slot_piece = lax.all_gather(slot_rows, "tp", axis=2, tiled=True)
    own_piece = lax.all_gather(routed_input[None], "tp", axis=2, tiled=True)
    own_rows = own_piece[0]
    gate_sum = jnp.einsum(
        "emc,ecf->emf", slot_piece, expert_gate, preferred_element_type=jnp.float32
    )
    up_sum = jnp.einsum("emc,ecf->emf", slot_piece, expert_up, preferred_element_type=jnp.float32)
    square_sum = jnp.sum(jnp.square(slot_piece.astype(jnp.float32)), axis=2)
    shared_gate_sum = jnp.dot(own_rows, shared_gate, preferred_element_type=jnp.float32)
    shared_up_sum = jnp.dot(own_rows, shared_up, preferred_element_type=jnp.float32)
    shared_square = jnp.sum(jnp.square(own_rows.astype(jnp.float32)), axis=1)
    full_width = expert_gate.shape[1]
    factor = lax.rsqrt(square_sum / full_width + NORM_EPS)[..., None]
    hidden = (jax.nn.silu(gate_sum * factor) * (up_sum * factor)).astype(jnp.bfloat16)
    shared_factor = lax.rsqrt(shared_square / full_width + NORM_EPS)[:, None]
    shared_hidden = (
        jax.nn.silu(shared_gate_sum * shared_factor) * (shared_up_sum * shared_factor)
    ).astype(jnp.bfloat16)
    shared_terms = jnp.dot(shared_hidden, shared_down, preferred_element_type=jnp.float32)
    routed_terms = jnp.einsum(
        "emf,efd->emd", hidden, expert_down, preferred_element_type=jnp.float32
    )
    routed_sum = lax.psum_scatter(
        routed_terms.astype(jnp.bfloat16), "tp", scatter_dimension=2, tiled=True
    ).astype(jnp.float32)
    return (routed_sum, shared_terms, placer)


def expert_finish(routed_sum, shared_sum, placer, route_weights):
    local_experts, slot_count, part_width = routed_sum.shape
    groups = lax.axis_size("ep")
    capacity = slot_count // groups
    leaving = jnp.transpose(
        routed_sum.astype(jnp.bfloat16).reshape(local_experts, groups, capacity, part_width),
        (1, 0, 2, 3),
    ).reshape(groups, local_experts * capacity, part_width)
    returned = lax.all_to_all(leaving, "ep", split_axis=0, concat_axis=0, tiled=True)
    copy_results = jnp.dot(
        placer,
        returned.reshape(groups * local_experts * capacity, part_width),
        preferred_element_type=jnp.float32,
    )
    row_count, top_count = route_weights.shape
    routed = jnp.sum(
        copy_results.reshape(row_count, top_count, part_width) * route_weights[:, :, None], axis=1
    )
    return (routed + shared_sum).astype(jnp.bfloat16)


def body(
    query_heads,
    key_heads,
    value_heads,
    diff_lambda,
    sub_gain,
    out_weight,
    routed_input,
    routes,
    route_weights,
    expert_gate,
    expert_up,
    expert_down,
    shared_gate,
    shared_up,
    shared_down,
):
    mixer_partial = mixer_terms(
        query_heads, key_heads, value_heads, diff_lambda, sub_gain, out_weight
    )
    routed_sum, shared_terms, placer = expert_terms(
        routed_input,
        routes,
        expert_gate,
        expert_up,
        expert_down,
        shared_gate,
        shared_up,
        shared_down,
    )
    mixer_sum, shared_sum = (
        lax.psum_scatter(
            mixer_partial.astype(jnp.bfloat16), "tp", scatter_dimension=1, tiled=True
        ).astype(jnp.float32),
        lax.psum_scatter(
            shared_terms.astype(jnp.bfloat16), "tp", scatter_dimension=1, tiled=True
        ).astype(jnp.float32),
    )
    return (
        mixer_sum.astype(jnp.bfloat16),
        expert_finish(routed_sum, shared_sum, placer, route_weights),
    )


def exchange(value, axis, swap):
    count = lax.axis_size(axis)
    return lax.ppermute(value, axis, [(i, swap(i)) for i in range(count)])


def to_partner(value):
    return exchange(value, "tp", lambda i: i ^ 1)


def along_z(value, step):
    return exchange(value, "tp", lambda i: i ^ (2 * step))


def along_ep(value, step):
    return exchange(value, "ep", lambda i: i ^ step)


def f32(value):
    return value.astype(jnp.float32)


def low(value):
    return value.astype(jnp.bfloat16)


def pair_sum(part):
    half = part.shape[0] // 2
    return f32(part[:half]) + f32(to_partner(part[half:]))


def z_sum(own, core):
    chips = lax.axis_size("tp") // 2
    chip = lax.axis_index("tp") // 2
    rows, width = own.shape
    wide = width // chips
    own = low(own)
    pieces = [
        along_z(lax.dynamic_slice(own, (0, (chip ^ step) * wide), (rows, wide)), step)
        for step in range(1, chips)
    ]
    total = f32(lax.dynamic_slice(own, (0, chip * wide), (rows, wide)))
    for piece in pieces:
        total = total + f32(piece)
    total = low(total)
    narrow = wide // 2
    other = to_partner(lax.dynamic_slice(total, (0, (1 - core) * narrow), (rows, narrow)))
    mine = lax.dynamic_slice(total, (0, core * narrow), (rows, narrow))
    first = jnp.where(core == 0, mine, other)
    second = jnp.where(core == 0, other, mine)
    return jnp.concatenate([first, second], axis=0)


def turn(value, core):
    half = value.shape[0] // 2
    first, second = value[:half], value[half:]
    return jnp.concatenate(
        [jnp.where(core == 0, first, second), jnp.where(core == 0, second, first)], axis=0
    )


def attend(query_heads, key_heads, value_heads, diff_lambda, sub_gain):
    row_count = query_heads.shape[0]
    local_heads = diff_lambda.shape[0]
    value_width = value_heads.shape[1] // local_heads
    key_width = query_heads.shape[1] // (2 * local_heads)
    groups = lax.axis_size("ep")
    index = lax.axis_index("ep")
    steps = jnp.arange(row_count, dtype=jnp.int32)
    positions = index * row_count + steps
    both = jnp.concatenate([query_heads, key_heads], axis=1)
    turned = low(
        rotate(f32(both).reshape(row_count, 4 * local_heads, key_width), positions)
    ).reshape(row_count, 4 * local_heads * key_width)
    query_rot = turned[:, : 2 * local_heads * key_width]
    own = jnp.concatenate([turned[:, 2 * local_heads * key_width :], value_heads], axis=1)
    blocks = [own] + [along_ep(own, step) for step in range(1, groups)]
    keys = jnp.concatenate(blocks, axis=0)
    key_positions = jnp.concatenate(
        [(index ^ step) * row_count + steps for step in range(groups)], axis=0
    )
    visible = key_positions[None, :] <= positions[:, None]
    outs = []
    value_start = 2 * local_heads * key_width
    for head in range(local_heads):
        values = keys[:, value_start + head * value_width : value_start + (head + 1) * value_width]
        maps = []
        for side in range(2):
            at = (2 * head + side) * key_width
            scores = lax.dot_general(
                query_rot[:, at : at + key_width],
                keys[:, at : at + key_width],
                (((1,), (1,)), ((), ())),
                preferred_element_type=jnp.float32,
            ) * (key_width ** (-0.5))
            scores = jnp.where(visible, scores, MASKED)
            maxima = jnp.max(scores, axis=1, keepdims=True)
            weights = jnp.exp(scores - maxima)
            totals = jnp.sum(weights, axis=1, keepdims=True)
            maps.append(
                jnp.dot(low(weights), values, preferred_element_type=jnp.float32) / totals
            )
        mixed = maps[0] - diff_lambda[head] * maps[1]
        outs.append(
            low(
                mixed
                * lax.rsqrt(jnp.mean(mixed * mixed, axis=1, keepdims=True) + NORM_EPS)
                * sub_gain
            )
        )
    return jnp.concatenate(outs, axis=1)


def gated(rows, gate, up, factor):
    gate_sum = jnp.dot(rows, gate, preferred_element_type=jnp.float32)
    up_sum = jnp.dot(rows, up, preferred_element_type=jnp.float32)
    return low(jax.nn.silu(gate_sum * factor) * (up_sum * factor))


def row_factor(rows):
    return lax.rsqrt(jnp.mean(jnp.square(f32(rows)), axis=1, keepdims=True) + NORM_EPS)


def dense_body(
    query_heads,
    key_heads,
    value_heads,
    diff_lambda,
    sub_gain,
    out_weight,
    routed_input,
    routes,
    route_weights,
    expert_gate,
    expert_up,
    expert_down,
    shared_gate,
    shared_up,
    shared_down,
):
    row_count, part_width = routed_input.shape
    half = row_count // 2
    quarter = half // 2
    chips = lax.axis_size("tp") // 2
    tp_index = lax.axis_index("tp")
    core, chip = tp_index % 2, tp_index // 2
    index = lax.axis_index("ep")
    gate, up, down = expert_gate[0], expert_up[0], expert_down[0]

    barrier = lax.optimization_barrier
    steps = range(1, chips)
    near = routed_input
    far = jnp.concatenate([along_z(near, step) for step in steps], axis=1)
    places = [(chip ^ step) * 2 + (core ^ side) for side in range(2) for step in range(chips)]

    def reorder(weight):
        return jnp.concatenate(
            [
                lax.dynamic_slice(weight, (place * part_width, 0), (part_width, weight.shape[1]))
                for place in places
            ],
            axis=0,
        )

    gate, up, first_gate, first_up = barrier(
        tuple(reorder(weight) for weight in (gate, up, shared_gate, shared_up))
    )

    def share(step):
        picked = jnp.sum(jnp.where(routes == (index ^ step), route_weights, 0.0), axis=1)
        picked = turn(picked, core)
        return (along_ep(picked, step) if step else picked)[:, None]

    shares = [share(step) for step in range(4)]

    def spread(piece):
        x_piece = along_ep(piece, 1)
        y_piece = along_ep(piece, 2)
        d_top = along_ep(x_piece[:half], 2)
        d_rest = along_ep(y_piece[half:], 1)
        return jnp.concatenate([x_piece, y_piece], axis=0), jnp.concatenate([d_top, d_rest], axis=0)

    def whole(first, second):
        return barrier(
            jnp.concatenate([first, second, to_partner(first), to_partner(second)], axis=1)
        )

    near_xy, near_d = spread(near)
    far_xy, far_d = spread(far)

    heads_out = attend(query_heads, key_heads, value_heads, diff_lambda, sub_gain)
    mixer_part = low(jnp.dot(turn(heads_out, core), out_weight, preferred_element_type=jnp.float32))
    mixer_output = z_sum(pair_sum(mixer_part), core)

    def hidden_of(rows):
        return barrier(gated(rows, gate, up, row_factor(rows)))

    def routed(hidden, weight):
        return jnp.dot(turn(hidden, core), down, preferred_element_type=jnp.float32) * weight

    own = whole(near, far)
    shared_hidden = barrier(gated(own, first_gate, first_up, row_factor(own)))
    shared_part = jnp.dot(
        turn(shared_hidden, core), shared_down, preferred_element_type=jnp.float32
    )
    own_sum = pair_sum(low(routed(hidden_of(own), shares[0]) + shared_part))
    xy_hidden = hidden_of(whole(near_xy, far_xy))
    x_sum = pair_sum(low(routed(xy_hidden[:row_count], shares[1])))
    y_sum = pair_sum(low(routed(xy_hidden[row_count:], shares[2])))
    d_rows, xy_hidden = barrier((whole(near_d, far_d), xy_hidden))
    d_sum = low(pair_sum(low(routed(hidden_of(d_rows), shares[3]))))
    d_sum, mixer_output = barrier((d_sum, mixer_output))
    x_first = along_ep(low(x_sum[:quarter]), 1)
    y_second = along_ep(low(y_sum[quarter:]), 2)
    y_more = along_ep(d_sum[:quarter], 1)
    x_more = along_ep(d_sum[quarter:], 2)
    y_first = along_ep(low(y_sum[:quarter] + f32(y_more)), 2)
    x_second = along_ep(low(x_sum[quarter:] + f32(x_more)), 1)
    from_x = jnp.concatenate([x_first, x_second], axis=0)
    from_y = jnp.concatenate([y_first, y_second], axis=0)
    routed_output = z_sum(own_sum + f32(from_x) + f32(from_y), core)
    return mixer_output, routed_output


def power_of_two(value):
    return value & (value - 1) == 0


def solution(mesh):
    dense = mesh.shape["ep"] == 4 and mesh.shape["tp"] % 2 == 0 and power_of_two(mesh.shape["tp"])

    def chosen(*arguments):
        fits = dense and arguments[9].shape[0] == 1 and arguments[6].shape[0] % 32 == 0
        return (dense_body if fits else body)(*arguments)

    placed = (
        P("ep", "tp"),
        P("ep", "tp"),
        P("ep", "tp"),
        P("tp"),
        P(),
        P("tp", None),
        P("ep", "tp"),
        P("ep", None),
        P("ep", None),
        P("ep", None, "tp"),
        P("ep", None, "tp"),
        P("ep", "tp", None),
        P(None, "tp"),
        P(None, "tp"),
        P("tp", None),
    )
    return jax.shard_map(
        chosen, mesh=mesh, in_specs=placed, out_specs=(P("ep", "tp"), P("ep", "tp")), check_vma=False
    )
```

```python
import jax
import jax.numpy as jnp
from jax import lax
from jax.experimental import pallas as pl
from jax.experimental.pallas import tpu as pltpu
from jax.sharding import PartitionSpec as P

ROPE_BASE = 10000.0
NORM_EPS = 1e-06
MASKED = -1e30


def rotate(values, positions):
    half_width = values.shape[-1] // 2
    inverse_freq = ROPE_BASE ** (-jnp.arange(half_width, dtype=jnp.float32) / half_width)
    angles = positions.astype(jnp.float32)[:, None] * inverse_freq[None, :]
    angles = angles.reshape((angles.shape[0],) + (1,) * (values.ndim - 2) + (half_width,))
    cosine = jnp.cos(angles)
    sine_part = jnp.sin(angles)
    lower = values[..., :half_width]
    upper = values[..., half_width:]
    return jnp.concatenate(
        [lower * cosine - upper * sine_part, upper * cosine + lower * sine_part], axis=-1
    )


def mixer_terms(query_heads, key_heads, value_heads, diff_lambda, sub_gain, out_weight):
    row_count = query_heads.shape[0]
    local_heads = diff_lambda.shape[0]
    value_width = value_heads.shape[1] // local_heads
    key_width = query_heads.shape[1] // (2 * local_heads)
    score_scale = key_width ** (-0.5)
    offset = lax.axis_index("ep") * row_count
    positions = offset + jnp.arange(row_count, dtype=jnp.int32)
    last_row = offset + row_count - 1
    query_rot = rotate(
        query_heads.astype(jnp.float32).reshape(row_count, local_heads, 2, key_width), positions
    ).astype(jnp.bfloat16)
    queries = jnp.transpose(query_rot, (1, 2, 0, 3))
    key_rot = (
        rotate(
            key_heads.astype(jnp.float32).reshape(row_count, local_heads, 2, key_width), positions
        )
        .astype(jnp.bfloat16)
        .reshape(row_count, local_heads * 2 * key_width)
    )
    start_state = (
        jnp.full((local_heads, 2, row_count), MASKED, jnp.float32),
        jnp.zeros((local_heads, 2, row_count), jnp.float32),
        jnp.zeros((local_heads, 2, row_count, value_width), jnp.float32),
    )
    carried = start_state
    key_piece = lax.all_gather(key_rot, "ep", axis=0, tiled=True)
    value_piece = lax.all_gather(value_heads, "ep", axis=0, tiled=True)
    piece_rows = key_piece.shape[0]
    key_block = 512
    block_count = piece_rows // key_block
    key_blocks = key_piece.reshape(block_count, key_block, local_heads, 2, key_width)
    value_blocks = value_piece.reshape(block_count, key_block, local_heads, value_width)

    def block_step(running, block_item):
        key_rows, value_rows, block_index = block_item
        block_start = block_index * key_block

        def attend_block(partial_state):
            maxima, totals, weighted = partial_state
            key_positions = block_start + jnp.arange(key_block, dtype=jnp.int32)
            visible = key_positions[None, :] <= positions[:, None]
            scores = (
                jnp.einsum("hmqd,khmd->hmqk", queries, key_rows, preferred_element_type=jnp.float32)
                * score_scale
            )
            scores = jnp.where(visible, scores, MASKED)
            new_maxima = jnp.maximum(maxima, jnp.max(scores, axis=3))
            exp_weights = jnp.where(visible, jnp.exp(scores - new_maxima[..., None]), 0.0)
            shrink = jnp.exp(maxima - new_maxima)
            new_totals = totals * shrink + jnp.sum(exp_weights, axis=3)
            update = jnp.einsum(
                "hmqk,khw->hmqw",
                exp_weights.astype(jnp.bfloat16),
                value_rows,
                preferred_element_type=jnp.float32,
            )
            return (new_maxima, new_totals, weighted * shrink[..., None] + update)

        return (
            lax.cond(
                block_start <= last_row, attend_block, lambda partial_state: partial_state, running
            ),
            None,
        )

    carried, _ = lax.scan(
        block_step, carried, (key_blocks, value_blocks, jnp.arange(block_count, dtype=jnp.int32))
    )
    maxima, totals, weighted = carried
    attended = weighted / totals[..., None]
    mixed_heads = attended[:, 0] - diff_lambda[:, None, None] * attended[:, 1]
    normed = (
        mixed_heads
        * lax.rsqrt(jnp.mean(mixed_heads * mixed_heads, axis=2, keepdims=True) + NORM_EPS)
        * sub_gain
    )
    heads_out = jnp.transpose(normed.astype(jnp.bfloat16), (1, 0, 2)).reshape(
        row_count, local_heads * value_width
    )
    return jnp.dot(heads_out, out_weight, preferred_element_type=jnp.float32)


def expert_terms(
    routed_input, routes, expert_gate, expert_up, expert_down, shared_gate, shared_up, shared_down
):
    row_count, part_width = routed_input.shape
    top_count = routes.shape[1]
    local_experts = expert_gate.shape[0]
    groups = lax.axis_size("ep")
    experts = local_experts * groups
    capacity = 2 * row_count * top_count // experts
    copies = row_count * top_count
    flat_routes = routes.reshape(copies)
    onehot = (flat_routes[:, None] == jnp.arange(experts, dtype=jnp.int32)[None, :]).astype(
        jnp.int32
    )
    rank_within = jnp.sum((jnp.cumsum(onehot, axis=0) - onehot) * onehot, axis=1)
    slot_index = flat_routes * capacity + rank_within
    placer = (
        slot_index[:, None] == jnp.arange(experts * capacity, dtype=jnp.int32)[None, :]
    ).astype(jnp.bfloat16)
    token_slots = jnp.sum(placer.reshape(row_count, top_count, experts * capacity), axis=1)
    outgoing = jnp.dot(token_slots.T, routed_input, preferred_element_type=jnp.float32).astype(
        jnp.bfloat16
    )
    arrived = lax.all_to_all(
        outgoing.reshape(groups, local_experts * capacity, part_width),
        "ep",
        split_axis=0,
        concat_axis=0,
        tiled=True,
    )
    slot_count = groups * capacity
    slot_rows = jnp.transpose(
        arrived.reshape(groups, local_experts, capacity, part_width), (1, 0, 2, 3)
    ).reshape(local_experts, slot_count, part_width)
    slot_piece = lax.all_gather(slot_rows, "tp", axis=2, tiled=True)
    own_piece = lax.all_gather(routed_input[None], "tp", axis=2, tiled=True)
    own_rows = own_piece[0]
    gate_sum = jnp.einsum(
        "emc,ecf->emf", slot_piece, expert_gate, preferred_element_type=jnp.float32
    )
    up_sum = jnp.einsum("emc,ecf->emf", slot_piece, expert_up, preferred_element_type=jnp.float32)
    square_sum = jnp.sum(jnp.square(slot_piece.astype(jnp.float32)), axis=2)
    shared_gate_sum = jnp.dot(own_rows, shared_gate, preferred_element_type=jnp.float32)
    shared_up_sum = jnp.dot(own_rows, shared_up, preferred_element_type=jnp.float32)
    shared_square = jnp.sum(jnp.square(own_rows.astype(jnp.float32)), axis=1)
    full_width = expert_gate.shape[1]
    factor = lax.rsqrt(square_sum / full_width + NORM_EPS)[..., None]
    hidden = (jax.nn.silu(gate_sum * factor) * (up_sum * factor)).astype(jnp.bfloat16)
    shared_factor = lax.rsqrt(shared_square / full_width + NORM_EPS)[:, None]
    shared_hidden = (
        jax.nn.silu(shared_gate_sum * shared_factor) * (shared_up_sum * shared_factor)
    ).astype(jnp.bfloat16)
    shared_terms = jnp.dot(shared_hidden, shared_down, preferred_element_type=jnp.float32)
    routed_terms = jnp.einsum(
        "emf,efd->emd", hidden, expert_down, preferred_element_type=jnp.float32
    )
    routed_sum = lax.psum_scatter(
        routed_terms.astype(jnp.bfloat16), "tp", scatter_dimension=2, tiled=True
    ).astype(jnp.float32)
    return (routed_sum, shared_terms, placer)


def expert_finish(routed_sum, shared_sum, placer, route_weights):
    local_experts, slot_count, part_width = routed_sum.shape
    groups = lax.axis_size("ep")
    capacity = slot_count // groups
    leaving = jnp.transpose(
        routed_sum.astype(jnp.bfloat16).reshape(local_experts, groups, capacity, part_width),
        (1, 0, 2, 3),
    ).reshape(groups, local_experts * capacity, part_width)
    returned = lax.all_to_all(leaving, "ep", split_axis=0, concat_axis=0, tiled=True)
    copy_results = jnp.dot(
        placer,
        returned.reshape(groups * local_experts * capacity, part_width),
        preferred_element_type=jnp.float32,
    )
    row_count, top_count = route_weights.shape
    routed = jnp.sum(
        copy_results.reshape(row_count, top_count, part_width) * route_weights[:, :, None], axis=1
    )
    return (routed + shared_sum).astype(jnp.bfloat16)


def body(
    query_heads,
    key_heads,
    value_heads,
    diff_lambda,
    sub_gain,
    out_weight,
    routed_input,
    routes,
    route_weights,
    expert_gate,
    expert_up,
    expert_down,
    shared_gate,
    shared_up,
    shared_down,
):
    mixer_partial = mixer_terms(
        query_heads, key_heads, value_heads, diff_lambda, sub_gain, out_weight
    )
    routed_sum, shared_terms, placer = expert_terms(
        routed_input,
        routes,
        expert_gate,
        expert_up,
        expert_down,
        shared_gate,
        shared_up,
        shared_down,
    )
    mixer_sum, shared_sum = (
        lax.psum_scatter(
            mixer_partial.astype(jnp.bfloat16), "tp", scatter_dimension=1, tiled=True
        ).astype(jnp.float32),
        lax.psum_scatter(
            shared_terms.astype(jnp.bfloat16), "tp", scatter_dimension=1, tiled=True
        ).astype(jnp.float32),
    )
    return (
        mixer_sum.astype(jnp.bfloat16),
        expert_finish(routed_sum, shared_sum, placer, route_weights),
    )


def exchange(value, axis, swap):
    count = lax.axis_size(axis)
    return lax.ppermute(value, axis, [(i, swap(i)) for i in range(count)])


def to_partner(value):
    return exchange(value, "tp", lambda i: i ^ 1)


def along_z(value, step):
    return exchange(value, "tp", lambda i: i ^ (2 * step))


def along_ep(value, step):
    return exchange(value, "ep", lambda i: i ^ step)


def f32(value):
    return value.astype(jnp.float32)


def low(value):
    return value.astype(jnp.bfloat16)


def pair_sum(part):
    half = part.shape[0] // 2
    return f32(part[:half]) + f32(to_partner(part[half:]))


def z_sum(own, core, after=None):
    chips = lax.axis_size("tp") // 2
    chip = lax.axis_index("tp") // 2
    rows, width = own.shape
    wide = width // chips
    own = low(own)
    pieces = [
        along_z(lax.dynamic_slice(own, (0, (chip ^ step) * wide), (rows, wide)), step)
        for step in range(1, chips)
    ]
    if after is not None:
        pieces, _ = lax.optimization_barrier((pieces, after))
    total = f32(lax.dynamic_slice(own, (0, chip * wide), (rows, wide)))
    for piece in pieces:
        total = total + f32(piece)
    total = low(total)
    narrow = wide // 2
    other = to_partner(lax.dynamic_slice(total, (0, (1 - core) * narrow), (rows, narrow)))
    mine = lax.dynamic_slice(total, (0, core * narrow), (rows, narrow))
    first = jnp.where(core == 0, mine, other)
    second = jnp.where(core == 0, other, mine)
    return jnp.concatenate([first, second], axis=0)


def turn(value, core):
    half = value.shape[0] // 2
    first, second = value[:half], value[half:]
    return jnp.concatenate(
        [jnp.where(core == 0, first, second), jnp.where(core == 0, second, first)], axis=0
    )


def copy_block(order_ref, in_ref, out_ref):
    out_ref[...] = in_ref[...]


def attend(query_heads, key_heads, value_heads, diff_lambda, sub_gain):
    row_count = query_heads.shape[0]
    local_heads = diff_lambda.shape[0]
    value_width = value_heads.shape[1] // local_heads
    key_width = query_heads.shape[1] // (2 * local_heads)
    groups = lax.axis_size("ep")
    index = lax.axis_index("ep")
    steps = jnp.arange(row_count, dtype=jnp.int32)
    positions = index * row_count + steps
    both = jnp.concatenate([query_heads, key_heads], axis=1)
    turned = low(
        rotate(f32(both).reshape(row_count, 4 * local_heads, key_width), positions)
    ).reshape(row_count, 4 * local_heads * key_width)
    query_rot = turned[:, : 2 * local_heads * key_width]
    own = jnp.concatenate([turned[:, 2 * local_heads * key_width :], value_heads], axis=1)
    blocks = [own] + [along_ep(own, step) for step in range(1, groups)]
    keys = jnp.concatenate(blocks, axis=0)
    key_positions = jnp.concatenate(
        [(index ^ step) * row_count + steps for step in range(groups)], axis=0
    )
    visible = key_positions[None, :] <= positions[:, None]
    outs = []
    value_start = 2 * local_heads * key_width
    for head in range(local_heads):
        values = keys[:, value_start + head * value_width : value_start + (head + 1) * value_width]
        maps = []
        for side in range(2):
            at = (2 * head + side) * key_width
            scores = lax.dot_general(
                query_rot[:, at : at + key_width],
                keys[:, at : at + key_width],
                (((1,), (1,)), ((), ())),
                preferred_element_type=jnp.float32,
            ) * (key_width ** (-0.5))
            scores = jnp.where(visible, scores, MASKED)
            maxima = jnp.max(scores, axis=1, keepdims=True)
            weights = jnp.exp(scores - maxima)
            totals = jnp.sum(weights, axis=1, keepdims=True)
            maps.append(
                jnp.dot(low(weights), values, preferred_element_type=jnp.float32) / totals
            )
        mixed = maps[0] - diff_lambda[head] * maps[1]
        outs.append(
            low(
                mixed
                * lax.rsqrt(jnp.mean(mixed * mixed, axis=1, keepdims=True) + NORM_EPS)
                * sub_gain
            )
        )
    return jnp.concatenate(outs, axis=1)


def gated(rows, gate, up, factor):
    gate_sum = jnp.dot(rows, gate, preferred_element_type=jnp.float32)
    up_sum = jnp.dot(rows, up, preferred_element_type=jnp.float32)
    return low(jax.nn.silu(gate_sum * factor) * (up_sum * factor))


def row_factor(rows):
    return lax.rsqrt(jnp.mean(jnp.square(f32(rows)), axis=1, keepdims=True) + NORM_EPS)


def dense_body(
    query_heads,
    key_heads,
    value_heads,
    diff_lambda,
    sub_gain,
    out_weight,
    routed_input,
    routes,
    route_weights,
    expert_gate,
    expert_up,
    expert_down,
    shared_gate,
    shared_up,
    shared_down,
):
    row_count, part_width = routed_input.shape
    half = row_count // 2
    quarter = half // 2
    chips = lax.axis_size("tp") // 2
    tp_index = lax.axis_index("tp")
    core, chip = tp_index % 2, tp_index // 2
    index = lax.axis_index("ep")
    gate, up, down = expert_gate[0], expert_up[0], expert_down[0]

    barrier = lax.optimization_barrier
    steps = range(1, chips)
    near = routed_input
    far = jnp.concatenate([along_z(near, step) for step in steps], axis=1)
    places = [(chip ^ step) * 2 + (core ^ side) for side in range(2) for step in range(chips)]

    places = jnp.stack(places).astype(jnp.int32)

    def reorder(weight):
        width = weight.shape[1]
        return pl.pallas_call(
            copy_block,
            grid_spec=pltpu.PrefetchScalarGridSpec(
                num_scalar_prefetch=1,
                grid=(2 * chips,),
                in_specs=[pl.BlockSpec((part_width, width), lambda k, order: (order[k], 0))],
                out_specs=pl.BlockSpec((part_width, width), lambda k, order: (k, 0)),
            ),
            out_shape=jax.ShapeDtypeStruct(weight.shape, weight.dtype),
            cost_estimate=pl.CostEstimate(
                flops=weight.size * 100, bytes_accessed=weight.size * 4, transcendentals=0
            ),
        )(places, weight)

    gate, up, first_gate, first_up = barrier(
        tuple(reorder(weight) for weight in (gate, up, shared_gate, shared_up))
    )

    def share(step):
        picked = jnp.sum(jnp.where(routes == (index ^ step), route_weights, 0.0), axis=1)
        picked = turn(picked, core)
        return (along_ep(picked, step) if step else picked)[:, None]

    shares = [share(step) for step in range(4)]

    def spread(piece):
        x_piece = along_ep(piece, 1)
        y_piece = along_ep(piece, 2)
        d_top = along_ep(x_piece[:half], 2)
        d_rest = along_ep(y_piece[half:], 1)
        return jnp.concatenate([x_piece, y_piece], axis=0), jnp.concatenate([d_top, d_rest], axis=0)

    def whole(first, second):
        return barrier(
            jnp.concatenate([first, second, to_partner(first), to_partner(second)], axis=1)
        )

    near_xy, near_d = spread(near)
    far_xy, far_d = spread(far)

    heads_out = attend(query_heads, key_heads, value_heads, diff_lambda, sub_gain)
    mixer_part = low(jnp.dot(turn(heads_out, core), out_weight, preferred_element_type=jnp.float32))
    mixer_sum = pair_sum(mixer_part)

    def hidden_of(rows):
        return barrier(gated(rows, gate, up, row_factor(rows)))

    def routed(hidden, weight):
        return jnp.dot(turn(hidden, core), down, preferred_element_type=jnp.float32) * weight

    own = whole(near, far)
    shared_hidden = barrier(gated(own, first_gate, first_up, row_factor(own)))
    shared_part = jnp.dot(
        turn(shared_hidden, core), shared_down, preferred_element_type=jnp.float32
    )
    own_sum = pair_sum(low(routed(hidden_of(own), shares[0]) + shared_part))
    xy_rows, mixer_sum = barrier((whole(near_xy, far_xy), mixer_sum))
    xy_hidden = hidden_of(xy_rows)
    x_sum = pair_sum(low(routed(xy_hidden[:row_count], shares[1])))
    y_sum = pair_sum(low(routed(xy_hidden[row_count:], shares[2])))
    d_rows, xy_hidden = barrier((whole(near_d, far_d), xy_hidden))
    d_sum = low(pair_sum(low(routed(hidden_of(d_rows), shares[3]))))
    mixer_output = z_sum(mixer_sum, core, d_sum)
    x_first = along_ep(low(x_sum[:quarter]), 1)
    y_second = along_ep(low(y_sum[quarter:]), 2)
    y_more = along_ep(d_sum[:quarter], 1)
    x_more = along_ep(d_sum[quarter:], 2)
    y_first = along_ep(low(y_sum[:quarter] + f32(y_more)), 2)
    x_second = along_ep(low(x_sum[quarter:] + f32(x_more)), 1)
    from_x = jnp.concatenate([x_first, x_second], axis=0)
    from_y = jnp.concatenate([y_first, y_second], axis=0)
    routed_output = z_sum(own_sum + f32(from_x) + f32(from_y), core)
    return mixer_output, routed_output


def power_of_two(value):
    return value & (value - 1) == 0


def solution(mesh):
    dense = mesh.shape["ep"] == 4 and mesh.shape["tp"] % 2 == 0 and power_of_two(mesh.shape["tp"])

    def chosen(*arguments):
        fits = dense and arguments[9].shape[0] == 1 and arguments[6].shape[0] % 32 == 0
        return (dense_body if fits else body)(*arguments)

    placed = (
        P("ep", "tp"),
        P("ep", "tp"),
        P("ep", "tp"),
        P("tp"),
        P(),
        P("tp", None),
        P("ep", "tp"),
        P("ep", None),
        P("ep", None),
        P("ep", None, "tp"),
        P("ep", None, "tp"),
        P("ep", "tp", None),
        P(None, "tp"),
        P(None, "tp"),
        P("tp", None),
    )
    return jax.shard_map(
        chosen, mesh=mesh, in_specs=placed, out_specs=(P("ep", "tp"), P("ep", "tp")), check_vma=False
    )
```
